32 devices in a mesh: ep: 4 (over y, x), tp: 8 (over z, core).
Axes of the slice: x: 2, y: 2, z: 4, core: 2. Of those that a mesh axis runs over, the one named last changes fastest.
Arguments:
- tokens: bfloat16 [2048, 4096], P('tp', 'ep'), may hold values from -20 to 20
- norm_gain: bfloat16 [4096], P('ep'), may hold values from 0.099609375 to 1.8984375
- expert_ids: int32 [2048, 2], P('tp'), may hold values from 0 to 7, all different within a row; in each aligned block of 256 rows (0 to 255, 256 to 511, ...) at most 128 rows name the same one
- combine_weight: float32 [2048, 2], P('tp'), may hold values from 0.05 to 1
- w_gate: bfloat16 [8, 2048, 4096], P('tp', 'ep'), may hold values from -0.09375 to 0.09375
- w_up: bfloat16 [8, 2048, 4096], P('tp', 'ep'), may hold values from -0.09375 to 0.09375
- w_down: bfloat16 [8, 2048, 4096], P('tp', None, 'ep'), may hold values from -2 to 2
- out_gain: bfloat16 [4096], P('ep'), may hold values from 0.099609375 to 1.8984375
Outputs:
- mixed: bfloat16 [2048, 4096], P('tp', 'ep')
The draws below stay inside these ranges and needn't reach their ends.
Inputs may be any that keep to these rules, and one draw needn't show every extreme that they name: `expert_ids`: each row names 2 different experts; among the rows of one index of tp no expert is named by more than 128 rows, a bound that some block reaches.
All inputs are finite; a program needn't handle non-finite values.
Results may differ from the reference program's by a relative error of at most 0.007.
Values may be sent and summed in bfloat16 or wider, within the bound.
A program may use at most 64 MiB of HBM per device.

```python
import math
import jax
import jax.numpy as jnp
import numpy as np
from jax import lax

D = 4096
F = 2048
TOP = 2
TOK_DEV = 256
EXPERTS = 8
TOKENS = 2048
CAP = 128
N_TP = 8


def draw_tokens(key, part):
    first, second, third = jax.random.split(key, 3)
    block_scale = jnp.exp(jax.random.uniform(first, (D // 64,), jnp.float32, -1.1, 1.1))
    column_scale = jnp.repeat(block_scale, 64)
    base = jnp.clip(jax.random.normal(second, (TOKENS, D), jnp.float32), -6.0, 6.0)
    values = base * column_scale[None, :]
    return values.astype(jnp.bfloat16)


def draw_w_down(key, part):
    first, second = jax.random.split(key, 2)
    block_scale = jnp.exp(jax.random.uniform(first, (D // 64,), jnp.float32, -1.0, 1.0))
    column_scale = jnp.repeat(block_scale, 64)
    base = jnp.clip(jax.random.normal(second, (EXPERTS, F, D), jnp.float32), -4.0, 4.0)
    values = base * F ** (-0.5) * column_scale[None, None, :]
    return values.astype(jnp.bfloat16)


def levels(rng, shape, pieces, low, top_value):
    loudness, own = 1.0, jax.random.fold_in(rng, 6)
    for dim, blocks in pieces:
        heights = jnp.exp(jax.random.uniform(jax.random.fold_in(own, dim), (blocks,), jnp.float32, low / len(pieces), top_value / len(pieces)))
        loudness = loudness * jnp.repeat(heights, shape[dim] // blocks).reshape([-1 if axis == dim else 1 for axis in range(len(shape))])
    return loudness


def deal_out(own_key, own, number, rows, amount, top, bound, skew):
    ranking = jax.random.permutation(own_key, amount)
    heavy_load, usual = load_shares(amount, rows * top, bound, skew, True), load_shares(amount, rows * top, bound, skew, False)
    places = jnp.arange(amount)

    def named(lengths, turn):
        used = int((lengths > 0).sum())
        fixed = max(1, used // 4)
        passed = fixed + (places - fixed + turn * (used - fixed)) % max(1, amount - fixed)
        return jnp.zeros((amount,), jnp.int32).at[ranking[jnp.where(places < fixed, places, passed)]].set(jnp.asarray(lengths, jnp.int32))

    lengths = jnp.where(number % 4 == 0, named(heavy_load, number // 4), named(usual, number - number // 4 - 1))
    mixed = jax.random.permutation(jax.random.fold_in(own, 3), amount)
    giver, taker = mixed[0:amount // 2 * 2:2], mixed[1:amount // 2 * 2:2]
    slack = jnp.minimum(lengths[giver] - 1, bound - lengths[taker]) // 2
    slack = jnp.where((giver == ranking[0]) | (taker == ranking[0]) | (lengths[taker] == 0), 0, jnp.maximum(slack, 0))
    passed = jax.random.randint(jax.random.fold_in(own, 4), (amount // 2,), 0, 1 << 20) % (slack + 1)
    lengths = lengths.at[giver].add(-passed).at[taker].add(passed)
    items = jnp.searchsorted(jnp.cumsum(lengths), jnp.arange(rows * top), side="right").astype(jnp.int32)
    table = items.reshape(top, rows).T
    table = table[jax.random.permutation(jax.random.fold_in(own, 1), rows)]
    turn = jax.random.randint(jax.random.fold_in(own, 2), (rows, 1), 0, top)
    return jnp.take_along_axis(table, (jnp.arange(top)[None, :] + turn) % top, axis=1)


def load_shares(number_of, total, bound, skew, full):
    loads = [(1 << 20) // math.isqrt(rank ** skew) + 1 for rank in range(1, number_of + 1)]
    largest = bound if full else min(bound, max(-(-total // number_of), total * loads[0] // sum(loads)))
    least = 1 if total - largest >= number_of - 1 else 0
    given, rest = [largest] + [least] * (number_of - 1), total - largest - least * (number_of - 1)
    while rest > 0:
        movable = [i for i in range(1, number_of) if given[i] < largest] or [i for i in range(1, number_of) if given[i] < bound]
        whole, left = sum([loads[i] for i in movable]), rest
        for i in movable:
            addition = min(bound - given[i], max(1, left * loads[i] // whole), rest)
            given[i] = given[i] + addition
            rest = rest - addition
    return np.array(given)


def bell_draw(stream_key, shape, width, bound, shards=(), kind=jnp.bfloat16):
    result = width * jax.random.normal(stream_key, shape, jnp.float32)
    if shards:
        result = result * levels(stream_key, shape, shards, -0.22, 0.18)
    return jnp.clip(result, -bound, bound).astype(kind)


def setup_inputs(seed: int = 0) -> dict:
    key_of = jax.random.split(jax.random.key(seed), 9)
    tokens = draw_tokens(jax.random.fold_in(key_of[8], 71), 0)
    norm_gain = jnp.clip(1.0 + 0.18 * jax.random.normal(key_of[1], (D,), jnp.float32), 0.099609375, 1.8984375).astype(jnp.bfloat16)
    expert_ids_keys = jax.random.split(jax.random.fold_in(key_of[2], 1), TOKENS // TOK_DEV)
    expert_ids_turns = jax.random.permutation(jax.random.fold_in(key_of[2], 3), TOKENS // TOK_DEV)
    expert_ids = jax.vmap(lambda own, number: deal_out(jax.random.fold_in(key_of[2], 2), own, number, TOK_DEV, EXPERTS, TOP, CAP, 2))(expert_ids_keys, expert_ids_turns).reshape((TOKENS, TOP))
    combine_weight = jnp.clip(jnp.exp(math.log(1.0) - 2.9957323 * jax.random.uniform(key_of[3], (TOKENS, TOP), jnp.float32) ** levels(key_of[3], (TOKENS, TOP), ((0, 8),), -0.2, 0.2)), 0.05, 1.0)
    w_gate = bell_draw(key_of[4], (EXPERTS, F, D), D ** -0.5, 0.09375, ((0, 8), (1, 4)))
    w_up = bell_draw(key_of[5], (EXPERTS, F, D), D ** -0.5, 0.09375, ((0, 8), (1, 4)))
    w_down = draw_w_down(jax.random.fold_in(key_of[8], 71), 0)
    out_gain = jnp.clip(1.0 + 0.18 * jax.random.normal(key_of[7], (D,), jnp.float32), 0.099609375, 1.8984375).astype(jnp.bfloat16)
    return dict(tokens=tokens, norm_gain=norm_gain, expert_ids=expert_ids, combine_weight=combine_weight, w_gate=w_gate, w_up=w_up, w_down=w_down, out_gain=out_gain)


epsilon = 1e-06

def reference(tokens, norm_gain, expert_ids, combine_weight, w_gate, w_up, w_down, out_gain):
    xf = tokens.astype(jnp.float32)
    normed = (xf * lax.rsqrt(lax.optimization_barrier(jnp.mean(xf * xf, axis=1, keepdims=True)) + epsilon) * norm_gain.astype(jnp.float32)).astype(jnp.bfloat16)
    flat_ids = expert_ids.reshape(-1)
    flat_weight = combine_weight.reshape(-1)
    source_rows = (jnp.arange(TOKENS * TOP, dtype=jnp.int32) // TOP).astype(jnp.int32)
    most = N_TP * CAP

    def one_expert(carry, expert):
        mask = flat_ids == expert
        ranks = jnp.cumsum(mask.astype(jnp.int32)) - 1
        slots = jnp.where(mask, ranks, most).astype(jnp.int32)
        rows = jnp.zeros((most + 1,), jnp.int32).at[slots].set(source_rows)[:most]
        weights = jnp.zeros((most + 1,), jnp.float32).at[slots].set(jnp.where(mask, flat_weight, 0.0))[:most]
        picked = normed[rows]
        gate = jnp.dot(picked, w_gate[expert].T, preferred_element_type=jnp.float32)
        up = jnp.dot(picked, w_up[expert].T, preferred_element_type=jnp.float32)
        hidden = (jax.nn.silu(gate) * up).astype(jnp.bfloat16)
        expert_out = jnp.dot(hidden, w_down[expert], preferred_element_type=jnp.float32).astype(jnp.bfloat16)
        carry = carry.at[rows].add(expert_out.astype(jnp.float32) * weights[:, None])
        return (carry, None)
    moe, _ = lax.scan(one_expert, jnp.zeros((TOKENS, D), jnp.float32), jnp.arange(EXPERTS, dtype=jnp.int32))
    mixed = moe * lax.rsqrt(lax.optimization_barrier(jnp.mean(moe * moe, axis=1, keepdims=True)) + epsilon) * out_gain.astype(jnp.float32)
    return mixed.astype(jnp.bfloat16)
```

```python
import functools
import math

import jax
import jax.numpy as jnp
from jax import lax
from jax.experimental import pallas as pl
from jax.experimental.pallas import tpu as pltpu
from jax.sharding import PartitionSpec as P

epsilon = 1e-06
MESH = pl.DeviceIdType.MESH
F32 = jnp.float32
BF16 = jnp.bfloat16


def remote(src, dst, send, recv, dev):
    return pltpu.make_async_remote_copy(
        src_ref=src, dst_ref=dst, send_sem=send, recv_sem=recv, device_id=dev, device_id_type=MESH
    )


def kernel(
    cfg, tok, gain, idst, cwt, og, wg, wu, wd, out,
    wgv, wuv, wdv, X, H, TB, O, R, G, SS, V, key, KS, KR, acc, wcol,
    wsem, lsend, lrecv, psend, precv, usend, urecv, ksend, krecv, rsend, rrecv, gsend, grecv, ssend, srecv, xsend, xrecv, hsend, hrecv,
):
    n_ep, n_tp, ny, nx, cap, crow, cols = cfg
    nch = n_tp * cap // crow
    grp = max(1, crow // cap)
    cut = max(1, cap // crow)
    piece = cap // cut
    half = crow // 2
    units = nch // cut
    T, wl = tok.shape
    pw = wl // cols
    top = idst.shape[0]
    width = wl * n_ep
    fl = wgv.shape[0]
    p = lax.axis_index("ep")
    q = lax.axis_index("tp")
    y, x = p // nx, p % nx

    weights = [
        pltpu.make_async_copy(a, b, wsem.at[k])
        for k, (a, b) in enumerate(((wg.at[0], wgv), (wu.at[0], wuv), (wd.at[0], wdv)))
    ]
    for w in weights:
        w.start()

    nz = n_tp // 2
    z, core = q // 2, q % 2

    def tpp(i):
        res, bit = 0, 1
        while bit < n_tp:
            res = res + ((q // bit + i // bit) % 2) * bit
            bit = bit * 2
        return res

    barrier = pltpu.get_barrier_semaphore()
    for j in range(1, n_ep):
        pl.semaphore_signal(barrier, inc=1, device_id=(lax.rem(p + j, n_ep), q), device_id_type=MESH)
    for i in range(1, n_tp):
        pl.semaphore_signal(barrier, inc=1, device_id=(p, tpp(i)), device_id_type=MESH)

    erow = lax.broadcasted_iota(jnp.int32, (n_tp, T), 0)
    named = jnp.zeros((n_tp, T), F32)
    for k in range(top):
        named = named + jnp.where(idst[k : k + 1, :] == erow, 1.0, 0.0)
    weight = jnp.zeros((128, T), F32)
    wrow = lax.broadcasted_iota(jnp.int32, (128, T), 0)
    for k in range(top):
        weight = weight + jnp.where(idst[k : k + 1, :] == wrow, cwt[k : k + 1, :], 0.0)
    wcol[...] = weight.T
    before = lax.broadcasted_iota(jnp.int32, (T, T), 0) < lax.broadcasted_iota(jnp.int32, (T, T), 1)
    rank = jnp.dot(named.astype(BF16), jnp.where(before, 1.0, 0.0).astype(BF16), preferred_element_type=F32)
    key[...] = jnp.where(named > 0.0, rank, -1.0)
    G[pl.ds(p, 1)] = jnp.broadcast_to(gain[...].astype(F32).reshape(1, wl), (8, wl))[None]

    def onehot(row):
        at = lax.broadcasted_iota(jnp.int32, (cap, T), 0).astype(F32)
        return jnp.where(row == at, 1.0, 0.0).astype(BF16)

    def pick(e):
        return onehot(key[pl.ds(e, 1), :])

    def rows_of(i):
        return pl.ds(pl.multiple_of(i * cap, cap), cap)

    def seek(table, k):
        res = k + table[0]
        for i in range(1, units):
            jump = table[i] - table[i - 1] - 1
            if jump:
                res = res + (k + units - i) // units * jump
        return res

    def line(head, tail):
        return head + [u for u in range(units) if u not in head + tail] + tail

    xorder = line([0, 1, 2], [3])
    horder = line([0, 2], [1, 3])
    reach = [0]
    for u in xorder:
        reach.append(max(reach[-1], (u * grp + grp - 1) // 2))

    def xchunk(t):
        return seek(xorder, t // cut) * cut + t % cut

    def hchunk(t):
        return seek(horder, t // cut) * cut + t % cut

    def part(j):
        return pl.ds(j * pw, pw)

    def keys(i):
        return remote(KS.at[i], KR.at[i], ksend.at[i], krecv.at[i], (p, tpp(i)))

    def right(s, j):
        b = TB.at[s, :, part(j)]
        return remote(b, b, lsend.at[s, j], lrecv.at[s, j], (p, lax.rem(q + 2, n_tp)))

    def left(s, j):
        b = TB.at[s, :, part(j)]
        return remote(b, b, usend.at[s, j], urecv.at[s, j], (p, lax.rem(q + n_tp - 2, n_tp)))

    def share(s, j):
        b = TB.at[s, :, part(j)]
        return remote(b, b, psend.at[s, j], precv.at[s, j], (p, z * 2 + 1 - core))

    def relay(k, j):
        @pl.when(z - k >= 0)
        def _():
            s = q - 2 * k
            right(s, j).wait_recv()

            @pl.when(z < nz - 1)
            def _():
                right(s, j).start()

            share(s, j).start()

        @pl.when(z + k < nz)
        def _():
            s = q + 2 * k
            left(s, j).wait_recv()

            @pl.when(z > 0)
            def _():
                left(s, j).start()

            share(s, j).start()

    def select(i, j):
        s = tpp(i)

        @pl.when(i % 2 == 1)
        def _():
            share(s, j).wait_recv()

        if j == 0:

            @pl.when(i > 0)
            def _():
                keys(i).wait_recv()

        row = KR[pl.ds(i, 1)][0, 0:1]
        block = jnp.dot(onehot(row), TB[pl.ds(s, 1), :, part(j)][0], preferred_element_type=F32)
        X[y, x, rows_of(i), part(j)] = block.astype(BF16)

    def fetch(k, j):
        lo = seek(reach[:-1], k) + 1
        hi = seek(reach[1:], k) + 1
        lax.fori_loop(lo, hi, lambda r, a: (relay(r, j), a)[1], 0)
        for g in range(grp):
            select(seek(xorder, k) * grp + g, j)

    def back(i, h):
        rows = pl.ds(pl.multiple_of(h * piece, piece), piece)
        return remote(O.at[i, rows], R.at[i, rows], rsend.at[i, h], rrecv.at[i, h], (p, tpp(i)))

    TB[pl.ds(q, 1)] = tok[...][None]
    KR[0] = jnp.broadcast_to(key[pl.ds(q, 1), :], (8, T))

    def key_rows(i, _):
        KS[pl.ds(i, 1)] = jnp.broadcast_to(key[pl.ds(tpp(i), 1), :], (8, T))[None]
        return 0

    lax.fori_loop(1, n_tp, key_rows, 0)
    for j in range(cols):
        select(0, j)
    pl.semaphore_wait(barrier, n_ep - 1 + n_tp - 1)

    def gcopy(j):
        return remote(G.at[p], G.at[p], gsend.at[j - 1], grecv.at[j - 1], (lax.rem(p + j, n_ep), q))

    def gwait(j):
        o = lax.rem(p - j + n_ep, n_ep)
        return remote(G.at[o], G.at[o], gsend.at[j - 1], grecv.at[j - 1], (lax.rem(p + j, n_ep), q))

    def gather(Z, ss, rs, wide):
        def ra(c):
            return pl.ds(pl.multiple_of(c * crow, half), half)

        def rb(c):
            return pl.ds(pl.multiple_of(c * crow + half, half), half)

        def send(k, c, n, j, r, dev):
            return remote(r, r, ss.at[k, c, n - 1, j], rs.at[k, c, n - 1, j], dev)

        def across(n):
            return (y * nx + lax.rem(x + n, nx), q)

        def along(n):
            return (lax.rem(y + n, ny) * nx + x, q)

        def first(c, mine, j=0):
            res = []
            w = pl.ds(j * wide, wide)
            for n in range(1, nx):
                o = x if mine else lax.rem(x - n + nx, nx)
                res.append(send(0, c, n, j, Z.at[y, o, ra(c), w], across(n)))
            for n in range(1, ny):
                o = y if mine else lax.rem(y - n + ny, ny)
                res.append(send(1, c, n, j, Z.at[o, x, rb(c), w], along(n)))
            return res

        def second(c, mine, j=0):
            res = []
            w = pl.ds(j * wide, wide)
            for n in range(1, ny):
                o = y if mine else lax.rem(y - n + ny, ny)
                res.append(send(2, c, n, j, Z.at[o, :, ra(c), w], along(n)))
            for n in range(1, nx):
                o = x if mine else lax.rem(x - n + nx, nx)
                res.append(send(3, c, n, j, Z.at[:, o, rb(c), w], across(n)))
            return res

        return first, second

    x1, x2 = gather(X, xsend, xrecv, wl)
    h1, h2 = gather(H, hsend, hrecv, fl)

    def start(copies):
        for c in copies:
            c.start()

    def recv(copies):
        for c in copies:
            c.wait_recv()

    def send_keys(i, _):
        keys(i).start()
        return 0

    lax.fori_loop(1, n_tp, send_keys, 0)
    for j in range(cols):

        @pl.when(z < nz - 1)
        def _():
            right(q, j).start()

        @pl.when(z > 0)
        def _():
            left(q, j).start()

        share(q, j).start()
        for g in range(1, grp):
            select(g, j)
        if j == 0 and grp == 1:
            start(x1(0, True))
    if grp > 1:
        start(x1(0, True))
    for j in range(1, n_ep):
        gcopy(j).start()
    acc[...] = jnp.zeros_like(acc)

    def crows(c):
        return pl.ds(pl.multiple_of(c * crow, crow), crow)

    def hidden(c):
        total = jnp.zeros((crow, 1), F32)
        for a in range(ny):
            for b in range(nx):
                v = X[a, b, crows(c)].astype(F32)
                total = total + jnp.sum(v * v, axis=1, keepdims=True)
        scale = lax.rsqrt(total / width + epsilon)
        for a in range(ny):
            for b in range(nx):
                o = a * nx + b
                v = X[a, b, crows(c)].astype(F32) * scale * G[o, 0:1]
                V[:, o * wl : (o + 1) * wl] = v.astype(BF16)
        dims = (((1,), (1,)), ((), ()))
        gate = lax.dot_general(V[...], wgv[...], dims, preferred_element_type=F32)
        up = lax.dot_general(V[...], wuv[...], dims, preferred_element_type=F32)
        H[y, x, crows(c)] = (gate / (1.0 + jnp.exp(-gate)) * up).astype(BF16)

    def down(c):
        res = jnp.zeros((crow, wl), F32)
        for a in range(ny):
            for b in range(nx):
                o = a * nx + b
                res = res + jnp.dot(H[a, b, crows(c)], wdv[o * fl : (o + 1) * fl, :], preferred_element_type=F32)
        return res.astype(BF16)

    def combine(i):
        e = tpp(i)
        lane = lax.broadcasted_iota(jnp.int32, (T, 128), 1)
        weight = jnp.sum(jnp.where(lane == e, wcol[...], 0.0), axis=1, keepdims=True)
        term = lax.dot_general(pick(e), R[i], (((0,), (0,)), ((), ())), preferred_element_type=F32)
        acc[...] += weight * term

    def step(t, _):
        @pl.when((t >= 8) & (t < nch + 8))
        def _():
            @pl.when(t == 8)
            def _():
                weights[2].wait()

            c = hchunk(t - 8)
            recv(h2(c, False))
            res = down(c)
            for g in range(grp):
                i = seek(horder, (t - 8) // cut) * grp + g
                h = (t - 8) % cut
                rows = pl.ds(pl.multiple_of(h * piece, piece), piece)
                O[pl.ds(i, 1), rows] = res[g * piece : (g + 1) * piece][None]

                @pl.when(i > 0)
                def _():
                    back(i, h).start()

                @pl.when(i == 0)
                def _():
                    R[0, rows] = res[g * piece : (g + 1) * piece]

        @pl.when((t >= 5) & (t < nch + 5))
        def _():
            @pl.when(t == 5)
            def _():
                weights[0].wait()
                weights[1].wait()
                for j in range(1, n_ep):
                    gwait(j).wait_recv()

            c = hchunk(t - 5)
            recv(x2(c, False))
            hidden(c)
            start(h1(c, True))

        @pl.when((t >= 6) & (t < nch + 6))
        def _():
            c = hchunk(t - 6)
            recv(h1(c, False))
            start(h2(c, True))

        @pl.when(t < nch)
        def _():
            @pl.when(t % cut == 0)
            def _():
                for j in range(cols):
                    fetch(t // cut, j)

            start(x1(xchunk(t), True))

        @pl.when((t >= 15) & (t < nch + 15) & ((t - 15) % cut == cut - 1))
        def _():
            for g in range(grp):
                i = seek(horder, (t - 15) // cut) * grp + g

                @pl.when(i > 0)
                def _():
                    for h in range(cut):
                        back(i, h).wait_recv()

                combine(i)

        @pl.when((t >= 1) & (t < nch + 1))
        def _():
            c = xchunk(t - 1)
            recv(x1(c, False))
            start(x2(c, True))

        return 0

    lax.fori_loop(1, nch + 15, step, 0)

    moe = acc[...]
    mine = jnp.sum(moe * moe, axis=1, keepdims=True)
    SS[pl.ds(p, 1)] = jnp.broadcast_to(mine, (T, 128)).T[0:8][None]

    def scopy(j, o):
        return remote(SS.at[o], SS.at[o], ssend.at[j - 1], srecv.at[j - 1], (lax.rem(p + j, n_ep), q))

    for j in range(1, n_ep):
        scopy(j, p).start()

    def drain_tp(i, _):
        keys(i).wait_send()
        for h in range(cut):
            back(i, h).wait_send()
        return 0

    lax.fori_loop(1, n_tp, drain_tp, 0)

    def drain_z(zs, _):
        s = zs * 2 + core
        for j in range(cols):
            share(s, j).wait_send()

            @pl.when((zs <= z) & (z < nz - 1))
            def _():
                right(s, j).wait_send()

            @pl.when((zs >= z) & (z > 0))
            def _():
                left(s, j).wait_send()

        return 0

    lax.fori_loop(0, nz, drain_z, 0)

    def drain_ep(c, _):
        for w in x1(c, True) + x2(c, True) + h1(c, True) + h2(c, True):
            w.wait_send()
        return 0

    lax.fori_loop(0, nch, drain_ep, 0)
    for j in range(1, n_ep):
        gcopy(j).wait_send()
    for j in range(1, n_ep):
        scopy(j, p).wait_send()
        scopy(j, lax.rem(p - j + n_ep, n_ep)).wait_recv()
    total = SS[0]
    for o in range(1, n_ep):
        total = total + SS[o]
    column = jnp.broadcast_to(total[0:1], (128, T)).T[:, 0:1]
    out[...] = (moe * lax.rsqrt(column / width + epsilon) * og[...].astype(F32).reshape(1, wl)).astype(BF16)


def body(tokens, norm_gain, expert_ids, combine_weight, w_gate, w_up, w_down, out_gain):
    T, wl = tokens.shape
    n_ep = lax.axis_size("ep")
    n_tp = lax.axis_size("tp")
    top = expert_ids.shape[1]
    cap = 2 * top * T // n_tp
    fl = w_gate.shape[1]
    width = wl * n_ep
    root = math.isqrt(n_ep)
    ny, nx = (root, root) if root * root == n_ep else (1, n_ep)
    rows = n_tp * cap
    crow = 64
    cut = max(1, cap // crow)
    nch = rows // crow
    peers = max(1, nx - 1, ny - 1)
    cols = 2 if wl % 256 == 0 else 1
    cfg = (n_ep, n_tp, ny, nx, cap, crow, cols)
    vm = pl.BlockSpec(memory_space=pltpu.VMEM)
    anym = pl.BlockSpec(memory_space=pl.ANY)
    dma = pltpu.SemaphoreType.DMA
    return pl.pallas_call(
        functools.partial(kernel, cfg),
        out_shape=jax.ShapeDtypeStruct((T, wl), BF16),
        in_specs=[vm] * 5 + [anym] * 3,
        out_specs=vm,
        scratch_shapes=[
            pltpu.VMEM((fl, width), BF16),
            pltpu.VMEM((fl, width), BF16),
            pltpu.VMEM((fl * n_ep, wl), BF16),
            pltpu.VMEM((ny, nx, rows, wl), BF16),
            pltpu.VMEM((ny, nx, rows, fl), BF16),
            pltpu.VMEM((n_tp, T, wl), BF16),
            pltpu.VMEM((n_tp, cap, wl), BF16),
            pltpu.VMEM((n_tp, cap, wl), BF16),
            pltpu.VMEM((n_ep, 8, wl), F32),
            pltpu.VMEM((n_ep, 8, T), F32),
            pltpu.VMEM((crow, width), BF16),
            pltpu.VMEM((n_tp, T), F32),
            pltpu.VMEM((n_tp, 8, T), F32),
            pltpu.VMEM((n_tp, 8, T), F32),
            pltpu.VMEM((T, wl), F32),
            pltpu.VMEM((T, 128), F32),
            dma((3,)),
            dma((n_tp, cols)), dma((n_tp, cols)), dma((n_tp, cols)), dma((n_tp, cols)),
            dma((n_tp, cols)), dma((n_tp, cols)), dma((n_tp,)), dma((n_tp,)),
            dma((n_tp, cut)), dma((n_tp, cut)),
            dma((n_ep,)), dma((n_ep,)), dma((n_ep,)), dma((n_ep,)),
            dma((4, nch, peers, 1)), dma((4, nch, peers, 1)), dma((4, nch, peers, 1)), dma((4, nch, peers, 1)),
        ],
        compiler_params=pltpu.CompilerParams(
            collective_id=0, has_side_effects=True, vmem_limit_bytes=60 * 1024 * 1024
        ),
        name="moe",
    )(
        tokens, norm_gain, expert_ids.T, combine_weight.T, out_gain,
        w_gate, w_up, w_down,
    )


def solution(mesh):
    return jax.shard_map(
        body,
        mesh=mesh,
        in_specs=(
            P("tp", "ep"),
            P("ep"),
            P("tp", None),
            P("tp", None),
            P("tp", "ep", None),
            P("tp", "ep", None),
            P("tp", None, "ep"),
            P("ep"),
        ),
        out_specs=P("tp", "ep"),
        check_vma=False,
    )
```

```python
import functools
import math

import jax
import jax.numpy as jnp
from jax import lax
from jax.experimental import pallas as pl
from jax.experimental.pallas import tpu as pltpu
from jax.sharding import PartitionSpec as P

epsilon = 1e-06
MESH = pl.DeviceIdType.MESH
F32 = jnp.float32
BF16 = jnp.bfloat16


def remote(src, dst, send, recv, dev):
    return pltpu.make_async_remote_copy(
        src_ref=src, dst_ref=dst, send_sem=send, recv_sem=recv, device_id=dev, device_id_type=MESH
    )


def kernel(
    cfg, tok, gain, idst, cwt, og, wg, wu, wd, out,
    wgv, wuv, wdv, X, H, TB, O, R, G, SS, V, WT, key, KS, KR, acc, wcol,
    wsem, lsend, lrecv, psend, precv, usend, urecv, ksend, krecv, rsend, rrecv, gsend, grecv, ssend, srecv, xsend, xrecv, hsend, hrecv,
):
    n_ep, n_tp, ny, nx, cap, crow, cols = cfg
    nch = n_tp * cap // crow
    grp = max(1, crow // cap)
    cut = max(1, cap // crow)
    piece = cap // cut
    half = crow // 2
    units = nch // cut
    T, wl = tok.shape
    pw = wl // cols
    top = idst.shape[0]
    width = wl * n_ep
    fl = wgv.shape[0]
    p = lax.axis_index("ep")
    q = lax.axis_index("tp")
    y, x = p // nx, p % nx

    weights = [
        pltpu.make_async_copy(a, b, wsem.at[k])
        for k, (a, b) in enumerate(((wg.at[0], wgv), (wu.at[0], wuv), (wd.at[0], wdv)))
    ]
    for w in weights:
        w.start()

    nz = n_tp // 2
    z, core = q // 2, q % 2

    def tpp(i):
        res, bit = 0, 1
        while bit < n_tp:
            res = res + ((q // bit + i // bit) % 2) * bit
            bit = bit * 2
        return res

    barrier = pltpu.get_barrier_semaphore()
    for j in range(1, n_ep):
        pl.semaphore_signal(barrier, inc=1, device_id=(lax.rem(p + j, n_ep), q), device_id_type=MESH)
    for i in range(1, n_tp):
        pl.semaphore_signal(barrier, inc=1, device_id=(p, tpp(i)), device_id_type=MESH)

    erow = lax.broadcasted_iota(jnp.int32, (n_tp, T), 0)
    named = jnp.zeros((n_tp, T), F32)
    for k in range(top):
        named = named + jnp.where(idst[k : k + 1, :] == erow, 1.0, 0.0)
    weight = jnp.zeros((128, T), F32)
    wrow = lax.broadcasted_iota(jnp.int32, (128, T), 0)
    for k in range(top):
        weight = weight + jnp.where(idst[k : k + 1, :] == wrow, cwt[k : k + 1, :], 0.0)
    wcol[...] = weight.T
    before = lax.broadcasted_iota(jnp.int32, (T, T), 0) < lax.broadcasted_iota(jnp.int32, (T, T), 1)
    rank = jnp.dot(named.astype(BF16), jnp.where(before, 1.0, 0.0).astype(BF16), preferred_element_type=F32)
    key[...] = jnp.where(named > 0.0, rank, -1.0)
    G[pl.ds(p, 1)] = jnp.broadcast_to(gain[...].astype(F32).reshape(1, wl), (8, wl))[None]

    def onehot(row):
        at = lax.broadcasted_iota(jnp.int32, (cap, T), 0).astype(F32)
        return jnp.where(row == at, 1.0, 0.0).astype(BF16)

    def pick(e):
        return onehot(key[pl.ds(e, 1), :])

    def rows_of(i):
        return pl.ds(pl.multiple_of(i * cap, cap), cap)

    def seek(table, k):
        res = k + table[0]
        for i in range(1, units):
            jump = table[i] - table[i - 1] - 1
            if jump:
                res = res + (k + units - i) // units * jump
        return res

    def line(head, tail):
        return head + [u for u in range(units) if u not in head + tail] + tail

    xorder = line([0, 1, 2], [3])
    horder = line([0, 2], [1, units - 1, 3])
    reach = [0]
    for u in xorder:
        reach.append(max(reach[-1], (u * grp + grp - 1) // 2))

    def xchunk(t):
        return seek(xorder, t // cut) * cut + t % cut

    def hchunk(t):
        return seek(horder, t // cut) * cut + t % cut

    def part(j):
        return pl.ds(j * pw, pw)

    def keys(i):
        return remote(KS.at[i], KR.at[i], ksend.at[i], krecv.at[i], (p, tpp(i)))

    def right(s, j):
        b = TB.at[s, :, part(j)]
        return remote(b, b, lsend.at[s, j], lrecv.at[s, j], (p, lax.rem(q + 2, n_tp)))

    def left(s, j):
        b = TB.at[s, :, part(j)]
        return remote(b, b, usend.at[s, j], urecv.at[s, j], (p, lax.rem(q + n_tp - 2, n_tp)))

    def share(s, j):
        b = TB.at[s, :, part(j)]
        return remote(b, b, psend.at[s, j], precv.at[s, j], (p, z * 2 + 1 - core))

    def relay(k, j):
        @pl.when(z - k >= 0)
        def _():
            s = q - 2 * k
            right(s, j).wait_recv()

            @pl.when(z < nz - 1)
            def _():
                right(s, j).start()

            share(s, j).start()

        @pl.when(z + k < nz)
        def _():
            s = q + 2 * k
            left(s, j).wait_recv()

            @pl.when(z > 0)
            def _():
                left(s, j).start()

            share(s, j).start()

    def select(i, j):
        s = tpp(i)

        @pl.when(i % 2 == 1)
        def _():
            share(s, j).wait_recv()

        if j == 0:

            @pl.when(i > 0)
            def _():
                keys(i).wait_recv()

        row = KR[pl.ds(i, 1)][0, 0:1]
        block = jnp.dot(onehot(row), TB[pl.ds(s, 1), :, part(j)][0], preferred_element_type=F32)
        X[y, x, rows_of(i), part(j)] = block.astype(BF16)

    def fetch(k, j):
        lo = seek(reach[:-1], k) + 1
        hi = seek(reach[1:], k) + 1
        lax.fori_loop(lo, hi, lambda r, a: (relay(r, j), a)[1], 0)
        for g in range(grp):
            select(seek(xorder, k) * grp + g, j)

    def back(i, h):
        rows = pl.ds(pl.multiple_of(h * piece, piece), piece)
        return remote(O.at[i, rows], R.at[i, rows], rsend.at[i, h], rrecv.at[i, h], (p, tpp(i)))

    TB[pl.ds(q, 1)] = tok[...][None]
    KR[0] = jnp.broadcast_to(key[pl.ds(q, 1), :], (8, T))

    def key_rows(i, _):
        KS[pl.ds(i, 1)] = jnp.broadcast_to(key[pl.ds(tpp(i), 1), :], (8, T))[None]
        return 0

    lax.fori_loop(1, n_tp, key_rows, 0)
    for j in range(cols):
        select(0, j)
    pl.semaphore_wait(barrier, n_ep - 1 + n_tp - 1)

    def gcopy(j):
        return remote(G.at[p], G.at[p], gsend.at[j - 1], grecv.at[j - 1], (lax.rem(p + j, n_ep), q))

    def gwait(j):
        o = lax.rem(p - j + n_ep, n_ep)
        return remote(G.at[o], G.at[o], gsend.at[j - 1], grecv.at[j - 1], (lax.rem(p + j, n_ep), q))

    def gather(Z, ss, rs, wide):
        def ra(c):
            return pl.ds(pl.multiple_of(c * crow, half), half)

        def rb(c):
            return pl.ds(pl.multiple_of(c * crow + half, half), half)

        def send(k, c, n, j, r, dev):
            return remote(r, r, ss.at[k, c, n - 1, j], rs.at[k, c, n - 1, j], dev)

        def across(n):
            return (y * nx + lax.rem(x + n, nx), q)

        def along(n):
            return (lax.rem(y + n, ny) * nx + x, q)

        def first(c, mine, j=0):
            res = []
            w = pl.ds(j * wide, wide)
            for n in range(1, nx):
                o = x if mine else lax.rem(x - n + nx, nx)
                res.append(send(0, c, n, j, Z.at[y, o, ra(c), w], across(n)))
            for n in range(1, ny):
                o = y if mine else lax.rem(y - n + ny, ny)
                res.append(send(1, c, n, j, Z.at[o, x, rb(c), w], along(n)))
            return res

        def second(c, mine, j=0):
            res = []
            w = pl.ds(j * wide, wide)
            for n in range(1, ny):
                o = y if mine else lax.rem(y - n + ny, ny)
                res.append(send(2, c, n, j, Z.at[o, :, ra(c), w], along(n)))
            for n in range(1, nx):
                o = x if mine else lax.rem(x - n + nx, nx)
                res.append(send(3, c, n, j, Z.at[:, o, rb(c), w], across(n)))
            return res

        return first, second

    x1, x2 = gather(X, xsend, xrecv, wl)
    h1, h2 = gather(H, hsend, hrecv, fl)

    def start(copies):
        for c in copies:
            c.start()

    def recv(copies):
        for c in copies:
            c.wait_recv()

    def send_keys(i, _):
        keys(i).start()
        return 0

    lax.fori_loop(1, n_tp, send_keys, 0)
    for j in range(cols):

        @pl.when(z < nz - 1)
        def _():
            right(q, j).start()

        @pl.when(z > 0)
        def _():
            left(q, j).start()

        share(q, j).start()
        for g in range(1, grp):
            select(g, j)
        if j == 0 and grp == 1:
            start(x1(0, True))
    if grp > 1:
        start(x1(0, True))
    for j in range(1, n_ep):
        gcopy(j).start()
    acc[...] = jnp.zeros_like(acc)

    def crows(c):
        return pl.ds(pl.multiple_of(c * crow, crow), crow)

    def hidden(c):
        total = jnp.zeros((crow, 1), F32)
        for a in range(ny):
            for b in range(nx):
                v = X[a, b, crows(c)].astype(F32)
                total = total + jnp.sum(v * v, axis=1, keepdims=True)
        scale = lax.rsqrt(total / width + epsilon)
        for a in range(ny):
            for b in range(nx):
                o = a * nx + b
                v = X[a, b, crows(c)].astype(F32) * scale * G[o, 0:1]
                V[:, o * wl : (o + 1) * wl] = v.astype(BF16)
        gate = jnp.dot(V[...], WT[0], preferred_element_type=F32)
        up = jnp.dot(V[...], WT[1], preferred_element_type=F32)
        H[y, x, crows(c)] = (gate / (1.0 + jnp.exp(-gate)) * up).astype(BF16)

    def down(c):
        res = jnp.zeros((crow, wl), F32)
        for a in range(ny):
            for b in range(nx):
                o = a * nx + b
                res = res + jnp.dot(H[a, b, crows(c)], wdv[o * fl : (o + 1) * fl, :], preferred_element_type=F32)
        return res.astype(BF16)

    def combine(i):
        e = tpp(i)
        lane = lax.broadcasted_iota(jnp.int32, (T, 128), 1)
        weight = jnp.sum(jnp.where(lane == e, wcol[...], 0.0), axis=1, keepdims=True)
        term = lax.dot_general(pick(e), R[i], (((0,), (0,)), ((), ())), preferred_element_type=F32)
        acc[...] += weight * term

    def step(t, _):
        @pl.when((t >= 5) & (t < nch + 5))
        def _():
            @pl.when(t == 5)
            def _():
                for j in range(1, n_ep):
                    gwait(j).wait_recv()

            c = hchunk(t - 5)
            recv(x2(c, False))
            hidden(c)
            start(h1(c, True))

        @pl.when(t < nch)
        def _():
            @pl.when(t % cut == 0)
            def _():
                for j in range(cols):
                    fetch(t // cut, j)

            start(x1(xchunk(t), True))

        @pl.when((t >= 8) & (t < nch + 8))
        def _():
            @pl.when(t == 8)
            def _():
                weights[2].wait()

            c = hchunk(t - 8)
            recv(h2(c, False))
            res = down(c)
            for g in range(grp):
                i = seek(horder, (t - 8) // cut) * grp + g
                h = (t - 8) % cut
                rows = pl.ds(pl.multiple_of(h * piece, piece), piece)
                O[pl.ds(i, 1), rows] = res[g * piece : (g + 1) * piece][None]

                @pl.when(i > 0)
                def _():
                    back(i, h).start()

                @pl.when(i == 0)
                def _():
                    R[0, rows] = res[g * piece : (g + 1) * piece]

        @pl.when((t >= 17) & (t < nch + 17) & ((t - 17) % cut == cut - 1))
        def _():
            for g in range(grp):
                i = seek(horder, (t - 17) // cut) * grp + g

                @pl.when(i > 0)
                def _():
                    for h in range(cut):
                        back(i, h).wait_recv()

                combine(i)

        @pl.when((t >= 6) & (t < nch + 6))
        def _():
            c = hchunk(t - 6)
            recv(h1(c, False))
            start(h2(c, True))

        @pl.when((t >= 1) & (t < nch + 1))
        def _():
            c = xchunk(t - 1)
            recv(x1(c, False))
            start(x2(c, True))

        @pl.when(t < 5)
        def _():
            @pl.when(t == 1)
            def _():
                weights[0].wait()
                weights[1].wait()

            def turn(b, _):
                at = pl.ds(pl.multiple_of((t - 1) * (width // 4) + b * 256, 256), 256)
                WT[0, at] = wgv[:, at].T
                WT[1, at] = wuv[:, at].T
                return 0

            lax.fori_loop(0, width // 1024, turn, 0)

        return 0

    lax.fori_loop(1, nch + 17, step, 0)

    moe = acc[...]
    mine = jnp.sum(moe * moe, axis=1, keepdims=True)
    SS[pl.ds(p, 1)] = jnp.broadcast_to(mine, (T, 128)).T[0:8][None]

    def scopy(j, o):
        return remote(SS.at[o], SS.at[o], ssend.at[j - 1], srecv.at[j - 1], (lax.rem(p + j, n_ep), q))

    for j in range(1, n_ep):
        scopy(j, p).start()

    def drain_tp(i, _):
        keys(i).wait_send()
        for h in range(cut):
            back(i, h).wait_send()
        return 0

    lax.fori_loop(1, n_tp, drain_tp, 0)

    def drain_z(zs, _):
        s = zs * 2 + core
        for j in range(cols):
            share(s, j).wait_send()

            @pl.when((zs <= z) & (z < nz - 1))
            def _():
                right(s, j).wait_send()

            @pl.when((zs >= z) & (z > 0))
            def _():
                left(s, j).wait_send()

        return 0

    lax.fori_loop(0, nz, drain_z, 0)

    def drain_ep(c, _):
        for w in x1(c, True) + x2(c, True) + h1(c, True) + h2(c, True):
            w.wait_send()
        return 0

    lax.fori_loop(0, nch, drain_ep, 0)
    for j in range(1, n_ep):
        gcopy(j).wait_send()
    for j in range(1, n_ep):
        scopy(j, p).wait_send()
        scopy(j, lax.rem(p - j + n_ep, n_ep)).wait_recv()
    total = SS[0]
    for o in range(1, n_ep):
        total = total + SS[o]
    column = jnp.broadcast_to(total[0:1], (128, T)).T[:, 0:1]
    out[...] = (moe * lax.rsqrt(column / width + epsilon) * og[...].astype(F32).reshape(1, wl)).astype(BF16)


def body(tokens, norm_gain, expert_ids, combine_weight, w_gate, w_up, w_down, out_gain):
    T, wl = tokens.shape
    n_ep = lax.axis_size("ep")
    n_tp = lax.axis_size("tp")
    top = expert_ids.shape[1]
    cap = 2 * top * T // n_tp
    fl = w_gate.shape[1]
    width = wl * n_ep
    root = math.isqrt(n_ep)
    ny, nx = (root, root) if root * root == n_ep else (1, n_ep)
    rows = n_tp * cap
    crow = 64
    cut = max(1, cap // crow)
    nch = rows // crow
    peers = max(1, nx - 1, ny - 1)
    cols = 2 if wl % 256 == 0 else 1
    cfg = (n_ep, n_tp, ny, nx, cap, crow, cols)
    vm = pl.BlockSpec(memory_space=pltpu.VMEM)
    anym = pl.BlockSpec(memory_space=pl.ANY)
    dma = pltpu.SemaphoreType.DMA
    return pl.pallas_call(
        functools.partial(kernel, cfg),
        out_shape=jax.ShapeDtypeStruct((T, wl), BF16),
        in_specs=[vm] * 5 + [anym] * 3,
        out_specs=vm,
        scratch_shapes=[
            pltpu.VMEM((fl, width), BF16),
            pltpu.VMEM((fl, width), BF16),
            pltpu.VMEM((fl * n_ep, wl), BF16),
            pltpu.VMEM((ny, nx, rows, wl), BF16),
            pltpu.VMEM((ny, nx, rows, fl), BF16),
            pltpu.VMEM((n_tp, T, wl), BF16),
            pltpu.VMEM((n_tp, cap, wl), BF16),
            pltpu.VMEM((n_tp, cap, wl), BF16),
            pltpu.VMEM((n_ep, 8, wl), F32),
            pltpu.VMEM((n_ep, 8, T), F32),
            pltpu.VMEM((crow, width), BF16),
            pltpu.VMEM((2, width, fl), BF16),
            pltpu.VMEM((n_tp, T), F32),
            pltpu.VMEM((n_tp, 8, T), F32),
            pltpu.VMEM((n_tp, 8, T), F32),
            pltpu.VMEM((T, wl), F32),
            pltpu.VMEM((T, 128), F32),
            dma((3,)),
            dma((n_tp, cols)), dma((n_tp, cols)), dma((n_tp, cols)), dma((n_tp, cols)),
            dma((n_tp, cols)), dma((n_tp, cols)), dma((n_tp,)), dma((n_tp,)),
            dma((n_tp, cut)), dma((n_tp, cut)),
            dma((n_ep,)), dma((n_ep,)), dma((n_ep,)), dma((n_ep,)),
            dma((4, nch, peers, 1)), dma((4, nch, peers, 1)), dma((4, nch, peers, 1)), dma((4, nch, peers, 1)),
        ],
        compiler_params=pltpu.CompilerParams(
            collective_id=0, has_side_effects=True, vmem_limit_bytes=60 * 1024 * 1024
        ),
        name="moe",
    )(
        tokens, norm_gain, expert_ids.T, combine_weight.T, out_gain,
        w_gate, w_up, w_down,
    )


def solution(mesh):
    return jax.shard_map(
        body,
        mesh=mesh,
        in_specs=(
            P("tp", "ep"),
            P("ep"),
            P("tp", None),
            P("tp", None),
            P("tp", "ep", None),
            P("tp", "ep", None),
            P("tp", None, "ep"),
            P("ep"),
        ),
        out_specs=P("tp", "ep"),
        check_vma=False,
    )
```

```python
import functools
import math

import jax
import jax.numpy as jnp
from jax import lax
from jax.experimental import pallas as pl
from jax.experimental.pallas import tpu as pltpu
from jax.sharding import PartitionSpec as P

epsilon = 1e-06
MESH = pl.DeviceIdType.MESH
F32 = jnp.float32
BF16 = jnp.bfloat16


def remote(src, dst, send, recv, dev):
    return pltpu.make_async_remote_copy(
        src_ref=src, dst_ref=dst, send_sem=send, recv_sem=recv, device_id=dev, device_id_type=MESH
    )


def kernel(
    cfg, tok, gain, idst, cwt, og, wg, wu, wd, out,
    wgv, wuv, wdv, X, H, TB, O, R, G, SS, V, WT, DB, key, KS, KR, acc, wcol,
    wsem, lsend, lrecv, psend, precv, usend, urecv, ksend, krecv, rsend, rrecv, gsend, grecv, ssend, srecv, xsend, xrecv, hsend, hrecv, dsend, drecv, msend, mrecv,
):
    n_ep, n_tp, ny, nx, cap, crow, cols, wb = cfg
    nch = n_tp * cap // crow
    grp = max(1, crow // cap)
    cut = max(1, cap // crow)
    piece = cap // cut
    units = nch // cut
    T, wl = tok.shape
    pw = wl // cols
    wa = wl - wb
    early = 4 if wb else 0
    top = idst.shape[0]
    width = wl * n_ep
    fl = wgv.shape[0]
    p = lax.axis_index("ep")
    q = lax.axis_index("tp")
    y, x = p // nx, p % nx

    weights = [
        pltpu.make_async_copy(a, b, wsem.at[k])
        for k, (a, b) in enumerate(((wg.at[0], wgv), (wu.at[0], wuv), (wd.at[0], wdv)))
    ]
    for w in weights:
        w.start()

    nz = n_tp // 2
    z, core = q // 2, q % 2

    def tpp(i):
        res, bit = 0, 1
        while bit < n_tp:
            res = res + ((q // bit + i // bit) % 2) * bit
            bit = bit * 2
        return res

    barrier = pltpu.get_barrier_semaphore()
    for j in range(1, n_ep):
        pl.semaphore_signal(barrier, inc=1, device_id=(lax.rem(p + j, n_ep), q), device_id_type=MESH)
    for i in range(1, n_tp):
        pl.semaphore_signal(barrier, inc=1, device_id=(p, tpp(i)), device_id_type=MESH)

    erow = lax.broadcasted_iota(jnp.int32, (n_tp, T), 0)
    named = jnp.zeros((n_tp, T), F32)
    for k in range(top):
        named = named + jnp.where(idst[k : k + 1, :] == erow, 1.0, 0.0)
    weight = jnp.zeros((128, T), F32)
    wrow = lax.broadcasted_iota(jnp.int32, (128, T), 0)
    for k in range(top):
        weight = weight + jnp.where(idst[k : k + 1, :] == wrow, cwt[k : k + 1, :], 0.0)
    wcol[...] = weight.T
    before = lax.broadcasted_iota(jnp.int32, (T, T), 0) < lax.broadcasted_iota(jnp.int32, (T, T), 1)
    rank = jnp.dot(named.astype(BF16), jnp.where(before, 1.0, 0.0).astype(BF16), preferred_element_type=F32)
    key[...] = jnp.where(named > 0.0, rank, -1.0)
    G[pl.ds(p, 1)] = jnp.broadcast_to(gain[...].astype(F32).reshape(1, wl), (8, wl))[None]

    def onehot(row):
        at = lax.broadcasted_iota(jnp.int32, (cap, T), 0).astype(F32)
        return jnp.where(row == at, 1.0, 0.0).astype(BF16)

    def pick(e):
        return onehot(key[pl.ds(e, 1), :])

    def rows_of(i):
        return pl.ds(pl.multiple_of(i * cap, cap), cap)

    def seek(table, k):
        res = k + table[0]
        for i in range(1, units):
            jump = table[i] - table[i - 1] - 1
            if jump:
                res = res + (k + units - i) // units * jump
        return res

    def line(head, tail):
        return head + [u for u in range(units) if u not in head + tail] + tail

    xorder = line([], [3])
    horder = line([0, 1], [units - 2, 2, units - 1, 3])
    reach = [0]
    for u in xorder:
        reach.append(max(reach[-1], (u * grp + grp - 1) // 2))

    def xchunk(t):
        return seek(xorder, t // cut) * cut + t % cut

    def hchunk(t):
        return seek(horder, t // cut) * cut + t % cut

    def part(j):
        return pl.ds(j * pw, pw)

    def keys(i):
        return remote(KS.at[i], KR.at[i], ksend.at[i], krecv.at[i], (p, tpp(i)))

    def right(s, j):
        b = TB.at[s, :, part(j)]
        return remote(b, b, lsend.at[s, j], lrecv.at[s, j], (p, lax.rem(q + 2, n_tp)))

    def left(s, j):
        b = TB.at[s, :, part(j)]
        return remote(b, b, usend.at[s, j], urecv.at[s, j], (p, lax.rem(q + n_tp - 2, n_tp)))

    def share(s, j):
        b = TB.at[s, :, part(j)]
        return remote(b, b, psend.at[s, j], precv.at[s, j], (p, z * 2 + 1 - core))

    def relay(k, j):
        @pl.when(z - k >= 0)
        def _():
            s = q - 2 * k
            right(s, j).wait_recv()

            @pl.when(z < nz - 1)
            def _():
                right(s, j).start()

            share(s, j).start()

        @pl.when(z + k < nz)
        def _():
            s = q + 2 * k
            left(s, j).wait_recv()

            @pl.when(z > 0)
            def _():
                left(s, j).start()

            share(s, j).start()

    def select(i, j):
        s = tpp(i)

        @pl.when(i % 2 == 1)
        def _():
            share(s, j).wait_recv()

        if j == 0:

            @pl.when(i > 0)
            def _():
                keys(i).wait_recv()

        row = KR[pl.ds(i, 1)][0, 0:1]
        block = jnp.dot(onehot(row), TB[pl.ds(s, 1), :, part(j)][0], preferred_element_type=F32)
        X[y, x, rows_of(i), part(j)] = block.astype(BF16)

    def fetch(k, j):
        lo = seek(reach[:-1], k) + 1
        hi = seek(reach[1:], k) + 1
        lax.fori_loop(lo, hi, lambda r, a: (relay(r, j), a)[1], 0)
        for g in range(grp):
            select(seek(xorder, k) * grp + g, j)

    def back(i, h):
        rows = pl.ds(pl.multiple_of(h * piece, piece), piece)
        return remote(O.at[i, rows], R.at[i, rows], rsend.at[i, h], rrecv.at[i, h], (p, tpp(i)))

    TB[pl.ds(q, 1)] = tok[...][None]
    if wb:
        DB[0, y, x] = tok[:, wa:]
    KR[0] = jnp.broadcast_to(key[pl.ds(q, 1), :], (8, T))

    def key_rows(i, _):
        KS[pl.ds(i, 1)] = jnp.broadcast_to(key[pl.ds(tpp(i), 1), :], (8, T))[None]
        return 0

    lax.fori_loop(1, n_tp, key_rows, 0)
    for j in range(cols):
        select(0, j)
    pl.semaphore_wait(barrier, n_ep - 1 + n_tp - 1)

    def gcopy(j):
        return remote(G.at[p], G.at[p], gsend.at[j - 1], grecv.at[j - 1], (lax.rem(p + j, n_ep), q))

    def gwait(j):
        o = lax.rem(p - j + n_ep, n_ep)
        return remote(G.at[o], G.at[o], gsend.at[j - 1], grecv.at[j - 1], (lax.rem(p + j, n_ep), q))

    def gather(Z, ss, rs, wide, rows):
        half = rows // 2

        def ra(c):
            return pl.ds(pl.multiple_of(c * rows, half), half)

        def rb(c):
            return pl.ds(pl.multiple_of(c * rows + half, half), half)

        def send(k, c, n, j, r, dev):
            return remote(r, r, ss.at[k, c, n - 1, j], rs.at[k, c, n - 1, j], dev)

        def across(n):
            return (y * nx + lax.rem(x + n, nx), q)

        def along(n):
            return (lax.rem(y + n, ny) * nx + x, q)

        def first(c, mine, j=0):
            res = []
            w = pl.ds(j * wide, wide)
            for n in range(1, nx):
                o = x if mine else lax.rem(x - n + nx, nx)
                res.append(send(0, c, n, j, Z.at[y, o, ra(c), w], across(n)))
            for n in range(1, ny):
                o = y if mine else lax.rem(y - n + ny, ny)
                res.append(send(1, c, n, j, Z.at[o, x, rb(c), w], along(n)))
            return res

        def second(c, mine, j=0):
            res = []
            w = pl.ds(j * wide, wide)
            for n in range(1, ny):
                o = y if mine else lax.rem(y - n + ny, ny)
                res.append(send(2, c, n, j, Z.at[o, :, ra(c), w], along(n)))
            for n in range(1, nx):
                o = x if mine else lax.rem(x - n + nx, nx)
                res.append(send(3, c, n, j, Z.at[:, o, rb(c), w], across(n)))
            return res

        return first, second

    thin = gather(X, xsend, xrecv, wa, crow)
    wide = gather(X, xsend, xrecv, wl, crow)
    h1, h2 = gather(H, hsend, hrecv, fl, crow)
    if wb:
        d1, d2 = gather(DB.at[0], dsend, drecv, wb, T)

    def move(act, k, c, mine):
        if wb == 0:
            act(wide[k](c, mine))
            return

        @pl.when(c // cut < early)
        def _():
            act(thin[k](c, mine))

        @pl.when(c // cut >= early)
        def _():
            act(wide[k](c, mine))

    def pass_on(src, dst, i):
        res = []
        for n in range(1, n_ep):
            o = lax.rem(p + n, n_ep)
            res.append(remote(DB.at[src, o // nx, o % nx], DB.at[dst, o // nx, o % nx], msend.at[dst, o], mrecv.at[dst, o], (p, tpp(i))))
        return res

    def blend(i):
        row = KR[pl.ds(i, 1)][0, 0:1]
        for n in range(1, n_ep):
            o = lax.rem(p + n, n_ep)
            block = jnp.dot(onehot(row), DB[pl.ds(i, 1), o // nx, o % nx][0], preferred_element_type=F32)
            X[o // nx, o % nx, rows_of(i), pl.ds(wa, wb)] = block.astype(BF16)

    def start(copies):
        for c in copies:
            c.start()

    def sent(copies):
        for c in copies:
            c.wait_send()

    def recv(copies):
        for c in copies:
            c.wait_recv()

    def send_keys(i, _):
        keys(i).start()
        return 0

    lax.fori_loop(1, n_tp, send_keys, 0)
    for j in range(cols):

        @pl.when(z < nz - 1)
        def _():
            right(q, j).start()

        @pl.when(z > 0)
        def _():
            left(q, j).start()

        share(q, j).start()
        for g in range(1, grp):
            select(g, j)
        if j == 0 and grp == 1:
            move(start, 0, 0, True)
            if wb:
                start(d1(0, True))
    if grp > 1:
        move(start, 0, 0, True)
    for j in range(1, n_ep):
        gcopy(j).start()
    acc[...] = jnp.zeros_like(acc)

    def crows(c):
        return pl.ds(pl.multiple_of(c * crow, crow), crow)

    def hidden(c):
        total = jnp.zeros((crow, 1), F32)
        for a in range(ny):
            for b in range(nx):
                v = X[a, b, crows(c)].astype(F32)
                total = total + jnp.sum(v * v, axis=1, keepdims=True)
        scale = lax.rsqrt(total / width + epsilon)
        for a in range(ny):
            for b in range(nx):
                o = a * nx + b
                v = X[a, b, crows(c)].astype(F32) * scale * G[o, 0:1]
                V[:, o * wl : (o + 1) * wl] = v.astype(BF16)
        gate = jnp.dot(V[...], WT[0], preferred_element_type=F32)
        up = jnp.dot(V[...], WT[1], preferred_element_type=F32)
        H[y, x, crows(c)] = (gate / (1.0 + jnp.exp(-gate)) * up).astype(BF16)

    def down(c):
        res = jnp.zeros((crow, wl), F32)
        for a in range(ny):
            for b in range(nx):
                o = a * nx + b
                res = res + jnp.dot(H[a, b, crows(c)], wdv[o * fl : (o + 1) * fl, :], preferred_element_type=F32)
        return res.astype(BF16)

    def combine(i):
        e = tpp(i)
        lane = lax.broadcasted_iota(jnp.int32, (T, 128), 1)
        weight = jnp.sum(jnp.where(lane == e, wcol[...], 0.0), axis=1, keepdims=True)
        term = lax.dot_general(pick(e), R[i], (((0,), (0,)), ((), ())), preferred_element_type=F32)
        acc[...] += weight * term

    def step(t, _):
        if wb:

            @pl.when(t == 3)
            def _():
                recv(d1(0, False))
                start(d2(0, True))

            @pl.when(t == 5)
            def _():
                recv(d2(0, False))
                start(pass_on(0, 1, 1))

            @pl.when(t == 9)
            def _():
                start(pass_on(0, 2, 2))

        @pl.when((t >= 6) & (t < nch + 6))
        def _():
            @pl.when(t == 6)
            def _():
                for j in range(1, n_ep):
                    gwait(j).wait_recv()

            c = hchunk(t - 6)
            move(recv, 1, c, False)
            if wb:

                @pl.when((c // cut < early) & (c % cut == 0))
                def _():
                    u = c // cut

                    @pl.when(u == 1)
                    def _():
                        recv(pass_on(0, 1, 1))

                    @pl.when(u == 2)
                    def _():
                        recv(pass_on(0, 2, 2))
                        start(pass_on(2, 3, 1))

                    @pl.when(u == 3)
                    def _():
                        recv(pass_on(2, 3, 1))

                    blend(u)

            hidden(c)
            start(h1(c, True))

        @pl.when(t < nch)
        def _():
            @pl.when(t % cut == 0)
            def _():
                for j in range(cols):
                    fetch(t // cut, j)

            move(start, 0, xchunk(t), True)

        @pl.when((t >= 9) & (t < nch + 9))
        def _():
            @pl.when(t == 9)
            def _():
                weights[2].wait()

            c = hchunk(t - 9)
            recv(h2(c, False))
            res = down(c)
            for g in range(grp):
                i = seek(horder, (t - 9) // cut) * grp + g
                h = (t - 9) % cut
                rows = pl.ds(pl.multiple_of(h * piece, piece), piece)
                O[pl.ds(i, 1), rows] = res[g * piece : (g + 1) * piece][None]

                @pl.when(i > 0)
                def _():
                    back(i, h).start()

                @pl.when(i == 0)
                def _():
                    R[0, rows] = res[g * piece : (g + 1) * piece]

        @pl.when((t >= 17) & (t < nch + 17) & ((t - 17) % cut == cut - 1))
        def _():
            for g in range(grp):
                i = seek(horder, (t - 17) // cut) * grp + g

                @pl.when(i > 0)
                def _():
                    for h in range(cut):
                        back(i, h).wait_recv()

                combine(i)

        @pl.when((t >= 7) & (t < nch + 7))
        def _():
            c = hchunk(t - 7)
            recv(h1(c, False))
            start(h2(c, True))

        @pl.when((t >= 1) & (t < nch + 1))
        def _():
            c = xchunk(t - 1)
            move(recv, 0, c, False)
            move(start, 1, c, True)

        @pl.when(t < 5)
        def _():
            @pl.when(t == 1)
            def _():
                weights[0].wait()
                weights[1].wait()

            def turn(b, _):
                at = pl.ds(pl.multiple_of((t - 1) * (width // 4) + b * 256, 256), 256)
                WT[0, at] = wgv[:, at].T
                WT[1, at] = wuv[:, at].T
                return 0

            lax.fori_loop(0, width // 1024, turn, 0)

        return 0

    lax.fori_loop(1, nch + 17, step, 0)

    moe = acc[...]
    mine = jnp.sum(moe * moe, axis=1, keepdims=True)
    SS[pl.ds(p, 1)] = jnp.broadcast_to(mine, (T, 128)).T[0:8][None]

    def scopy(j, o):
        return remote(SS.at[o], SS.at[o], ssend.at[j - 1], srecv.at[j - 1], (lax.rem(p + j, n_ep), q))

    for j in range(1, n_ep):
        scopy(j, p).start()

    def drain_tp(i, _):
        keys(i).wait_send()
        for h in range(cut):
            back(i, h).wait_send()
        return 0

    lax.fori_loop(1, n_tp, drain_tp, 0)

    def drain_z(zs, _):
        s = zs * 2 + core
        for j in range(cols):
            share(s, j).wait_send()

            @pl.when((zs <= z) & (z < nz - 1))
            def _():
                right(s, j).wait_send()

            @pl.when((zs >= z) & (z > 0))
            def _():
                left(s, j).wait_send()

        return 0

    lax.fori_loop(0, nz, drain_z, 0)

    def drain_ep(c, _):
        move(sent, 0, c, True)
        move(sent, 1, c, True)
        sent(h1(c, True) + h2(c, True))
        return 0

    lax.fori_loop(0, nch, drain_ep, 0)
    if wb:
        sent(d1(0, True) + d2(0, True) + pass_on(0, 1, 1) + pass_on(0, 2, 2) + pass_on(2, 3, 1))
    for j in range(1, n_ep):
        gcopy(j).wait_send()
    for j in range(1, n_ep):
        scopy(j, p).wait_send()
        scopy(j, lax.rem(p - j + n_ep, n_ep)).wait_recv()
    total = SS[0]
    for o in range(1, n_ep):
        total = total + SS[o]
    column = jnp.broadcast_to(total[0:1], (128, T)).T[:, 0:1]
    out[...] = (moe * lax.rsqrt(column / width + epsilon) * og[...].astype(F32).reshape(1, wl)).astype(BF16)


def body(tokens, norm_gain, expert_ids, combine_weight, w_gate, w_up, w_down, out_gain):
    T, wl = tokens.shape
    n_ep = lax.axis_size("ep")
    n_tp = lax.axis_size("tp")
    top = expert_ids.shape[1]
    cap = 2 * top * T // n_tp
    fl = w_gate.shape[1]
    width = wl * n_ep
    root = math.isqrt(n_ep)
    ny, nx = (root, root) if root * root == n_ep else (1, n_ep)
    rows = n_tp * cap
    crow = 64
    cut = max(1, cap // crow)
    nch = rows // crow
    peers = max(1, nx - 1, ny - 1)
    cols = 2 if wl % 256 == 0 else 1
    wb = wl * 5 // 8 // 128 * 128 if cap >= crow else 0
    cfg = (n_ep, n_tp, ny, nx, cap, crow, cols, wb)
    vm = pl.BlockSpec(memory_space=pltpu.VMEM)
    anym = pl.BlockSpec(memory_space=pl.ANY)
    dma = pltpu.SemaphoreType.DMA
    return pl.pallas_call(
        functools.partial(kernel, cfg),
        out_shape=jax.ShapeDtypeStruct((T, wl), BF16),
        in_specs=[vm] * 5 + [anym] * 3,
        out_specs=vm,
        scratch_shapes=[
            pltpu.VMEM((fl, width), BF16),
            pltpu.VMEM((fl, width), BF16),
            pltpu.VMEM((fl * n_ep, wl), BF16),
            pltpu.VMEM((ny, nx, rows, wl), BF16),
            pltpu.VMEM((ny, nx, rows, fl), BF16),
            pltpu.VMEM((n_tp, T, wl), BF16),
            pltpu.VMEM((n_tp, cap, wl), BF16),
            pltpu.VMEM((n_tp, cap, wl), BF16),
            pltpu.VMEM((n_ep, 8, wl), F32),
            pltpu.VMEM((n_ep, 8, T), F32),
            pltpu.VMEM((crow, width), BF16),
            pltpu.VMEM((2, width, fl), BF16),
            pltpu.VMEM((4, ny, nx, T, wb) if wb else (8, 128), BF16),
            pltpu.VMEM((n_tp, T), F32),
            pltpu.VMEM((n_tp, 8, T), F32),
            pltpu.VMEM((n_tp, 8, T), F32),
            pltpu.VMEM((T, wl), F32),
            pltpu.VMEM((T, 128), F32),
            dma((3,)),
            dma((n_tp, cols)), dma((n_tp, cols)), dma((n_tp, cols)), dma((n_tp, cols)),
            dma((n_tp, cols)), dma((n_tp, cols)), dma((n_tp,)), dma((n_tp,)),
            dma((n_tp, cut)), dma((n_tp, cut)),
            dma((n_ep,)), dma((n_ep,)), dma((n_ep,)), dma((n_ep,)),
            dma((4, nch, peers, 1)), dma((4, nch, peers, 1)), dma((4, nch, peers, 1)), dma((4, nch, peers, 1)),
            dma((4, 1, peers, 1)), dma((4, 1, peers, 1)), dma((4, n_ep)), dma((4, n_ep)),
        ],
        compiler_params=pltpu.CompilerParams(
            collective_id=0, has_side_effects=True, vmem_limit_bytes=60 * 1024 * 1024
        ),
        name="moe",
    )(
        tokens, norm_gain, expert_ids.T, combine_weight.T, out_gain,
        w_gate, w_up, w_down,
    )


def solution(mesh):
    return jax.shard_map(
        body,
        mesh=mesh,
        in_specs=(
            P("tp", "ep"),
            P("ep"),
            P("tp", None),
            P("tp", None),
            P("tp", "ep", None),
            P("tp", "ep", None),
            P("tp", None, "ep"),
            P("ep"),
        ),
        out_specs=P("tp", "ep"),
        check_vma=False,
    )
```

```python
import functools
import math

import jax
import jax.numpy as jnp
from jax import lax
from jax.experimental import pallas as pl
from jax.experimental.pallas import tpu as pltpu
from jax.sharding import PartitionSpec as P

epsilon = 1e-06
MESH = pl.DeviceIdType.MESH
F32 = jnp.float32
BF16 = jnp.bfloat16


def remote(src, dst, send, recv, dev):
    return pltpu.make_async_remote_copy(
        src_ref=src, dst_ref=dst, send_sem=send, recv_sem=recv, device_id=dev, device_id_type=MESH
    )


def kernel(
    cfg, tok, gain, idst, cwt, og, wg, wu, wd, out,
    wgv, wuv, wdv, X, H, TB, O, R, G, SS, V, WT, DB, key, KS, KR, acc, wcol,
    wsem, lsend, lrecv, psend, precv, usend, urecv, ksend, krecv, rsend, rrecv, gsend, grecv, ssend, srecv, xsend, xrecv, hsend, hrecv, dsend, drecv, msend, mrecv,
):
    n_ep, n_tp, ny, nx, cap, crow, cols, wb = cfg
    nch = n_tp * cap // crow
    grp = max(1, crow // cap)
    cut = max(1, cap // crow)
    piece = cap // cut
    units = nch // cut
    T, wl = tok.shape
    pw = wl // cols
    wa = wl - wb
    early = 4 if wb else 0
    top = idst.shape[0]
    width = wl * n_ep
    fl = wgv.shape[0]
    p = lax.axis_index("ep")
    q = lax.axis_index("tp")
    y, x = p // nx, p % nx

    weights = [
        pltpu.make_async_copy(a, b, wsem.at[k])
        for k, (a, b) in enumerate(((wg.at[0], wgv), (wu.at[0], wuv), (wd.at[0], wdv)))
    ]
    for w in weights:
        w.start()

    nz = n_tp // 2
    z, core = q // 2, q % 2

    def tpp(i):
        res, bit = 0, 1
        while bit < n_tp:
            res = res + ((q // bit + i // bit) % 2) * bit
            bit = bit * 2
        return res

    barrier = pltpu.get_barrier_semaphore()
    for j in range(1, n_ep):
        pl.semaphore_signal(barrier, inc=1, device_id=(lax.rem(p + j, n_ep), q), device_id_type=MESH)
    for i in range(1, n_tp):
        pl.semaphore_signal(barrier, inc=1, device_id=(p, tpp(i)), device_id_type=MESH)

    erow = lax.broadcasted_iota(jnp.int32, (n_tp, T), 0)
    named = jnp.zeros((n_tp, T), F32)
    for k in range(top):
        named = named + jnp.where(idst[k : k + 1, :] == erow, 1.0, 0.0)
    weight = jnp.zeros((128, T), F32)
    wrow = lax.broadcasted_iota(jnp.int32, (128, T), 0)
    for k in range(top):
        weight = weight + jnp.where(idst[k : k + 1, :] == wrow, cwt[k : k + 1, :], 0.0)
    wcol[...] = weight.T
    before = lax.broadcasted_iota(jnp.int32, (T, T), 0) < lax.broadcasted_iota(jnp.int32, (T, T), 1)
    rank = jnp.dot(named.astype(BF16), jnp.where(before, 1.0, 0.0).astype(BF16), preferred_element_type=F32)
    key[...] = jnp.where(named > 0.0, rank, -1.0)
    G[pl.ds(p, 1)] = jnp.broadcast_to(gain[...].astype(F32).reshape(1, wl), (8, wl))[None]

    def onehot(row):
        at = lax.broadcasted_iota(jnp.int32, (cap, T), 0).astype(F32)
        return jnp.where(row == at, 1.0, 0.0).astype(BF16)

    def pick(e):
        return onehot(key[pl.ds(e, 1), :])

    def rows_of(i):
        return pl.ds(pl.multiple_of(i * cap, cap), cap)

    def seek(table, k):
        res = k + table[0]
        for i in range(1, units):
            jump = table[i] - table[i - 1] - 1
            if jump:
                res = res + (k + units - i) // units * jump
        return res

    def line(head, tail):
        return head + [u for u in range(units) if u not in head + tail] + tail

    xorder = line([], [3])
    horder = line([0, 1], [units - 2, 2, units - 1, 3])
    reach = [0]
    for u in xorder:
        reach.append(max(reach[-1], (u * grp + grp - 1) // 2))

    def xchunk(t):
        return seek(xorder, t // cut) * cut + t % cut

    def hchunk(t):
        return seek(horder, t // cut) * cut + t % cut

    def part(j):
        return pl.ds(j * pw, pw)

    def keys(i):
        return remote(KS.at[i], KR.at[i], ksend.at[i], krecv.at[i], (p, tpp(i)))

    def right(s, j):
        b = TB.at[s, :, part(j)]
        return remote(b, b, lsend.at[s, j], lrecv.at[s, j], (p, lax.rem(q + 2, n_tp)))

    def left(s, j):
        b = TB.at[s, :, part(j)]
        return remote(b, b, usend.at[s, j], urecv.at[s, j], (p, lax.rem(q + n_tp - 2, n_tp)))

    def share(s, j):
        b = TB.at[s, :, part(j)]
        return remote(b, b, psend.at[s, j], precv.at[s, j], (p, z * 2 + 1 - core))

    def relay(k, j):
        @pl.when(z - k >= 0)
        def _():
            s = q - 2 * k
            right(s, j).wait_recv()

            @pl.when(z < nz - 1)
            def _():
                right(s, j).start()

            share(s, j).start()

        @pl.when(z + k < nz)
        def _():
            s = q + 2 * k
            left(s, j).wait_recv()

            @pl.when(z > 0)
            def _():
                left(s, j).start()

            share(s, j).start()

    def select(i, j):
        s = tpp(i)

        @pl.when(i % 2 == 1)
        def _():
            share(s, j).wait_recv()

        if j == 0:

            @pl.when(i > 0)
            def _():
                keys(i).wait_recv()

        row = KR[pl.ds(i, 1)][0, 0:1]
        block = jnp.dot(onehot(row), TB[pl.ds(s, 1), :, part(j)][0], preferred_element_type=F32)
        X[y, x, rows_of(i), part(j)] = block.astype(BF16)

    def fetch(k, j):
        lo = seek(reach[:-1], k) + 1
        hi = seek(reach[1:], k) + 1
        lax.fori_loop(lo, hi, lambda r, a: (relay(r, j), a)[1], 0)
        for g in range(grp):
            select(seek(xorder, k) * grp + g, j)

    def back(i, h):
        rows = pl.ds(pl.multiple_of(h * piece, piece), piece)
        return remote(O.at[i, rows], R.at[i, rows], rsend.at[i, h], rrecv.at[i, h], (p, tpp(i)))

    TB[pl.ds(q, 1)] = tok[...][None]
    if wb:
        DB[0, y, x] = tok[:, wa:]
    KR[0] = jnp.broadcast_to(key[pl.ds(q, 1), :], (8, T))

    def key_rows(i, _):
        KS[pl.ds(i, 1)] = jnp.broadcast_to(key[pl.ds(tpp(i), 1), :], (8, T))[None]
        return 0

    lax.fori_loop(1, n_tp, key_rows, 0)
    for j in range(cols):
        select(0, j)
    pl.semaphore_wait(barrier, n_ep - 1 + n_tp - 1)

    def gcopy(j):
        return remote(G.at[p], G.at[p], gsend.at[j - 1], grecv.at[j - 1], (lax.rem(p + j, n_ep), q))

    def gwait(j):
        o = lax.rem(p - j + n_ep, n_ep)
        return remote(G.at[o], G.at[o], gsend.at[j - 1], grecv.at[j - 1], (lax.rem(p + j, n_ep), q))

    def gather(Z, ss, rs, wide, rows):
        half = rows // 2

        def ra(c):
            return pl.ds(pl.multiple_of(c * rows, half), half)

        def rb(c):
            return pl.ds(pl.multiple_of(c * rows + half, half), half)

        def send(k, c, n, j, r, dev):
            return remote(r, r, ss.at[k, c, n - 1, j], rs.at[k, c, n - 1, j], dev)

        def across(n):
            return (y * nx + lax.rem(x + n, nx), q)

        def along(n):
            return (lax.rem(y + n, ny) * nx + x, q)

        def first(c, mine, j=0):
            res = []
            w = pl.ds(j * wide, wide)
            for n in range(1, nx):
                o = x if mine else lax.rem(x - n + nx, nx)
                res.append(send(0, c, n, j, Z.at[y, o, ra(c), w], across(n)))
            for n in range(1, ny):
                o = y if mine else lax.rem(y - n + ny, ny)
                res.append(send(1, c, n, j, Z.at[o, x, rb(c), w], along(n)))
            return res

        def second(c, mine, j=0):
            res = []
            w = pl.ds(j * wide, wide)
            for n in range(1, ny):
                o = y if mine else lax.rem(y - n + ny, ny)
                res.append(send(2, c, n, j, Z.at[o, :, ra(c), w], along(n)))
            for n in range(1, nx):
                o = x if mine else lax.rem(x - n + nx, nx)
                res.append(send(3, c, n, j, Z.at[:, o, rb(c), w], across(n)))
            return res

        return first, second

    thin = gather(X, xsend, xrecv, wa, crow)
    wide = gather(X, xsend, xrecv, wl, crow)
    h1, h2 = gather(H, hsend, hrecv, fl, crow)
    if wb:
        d1, d2 = gather(DB.at[0], dsend, drecv, wb, T)

    def move(act, k, c, mine):
        if wb == 0:
            act(wide[k](c, mine))
            return

        @pl.when(c // cut < early)
        def _():
            act(thin[k](c, mine))

        @pl.when(c // cut >= early)
        def _():
            act(wide[k](c, mine))

    def pass_on(src, dst, i):
        res = []
        for n in range(1, n_ep):
            o = lax.rem(p + n, n_ep)
            res.append(remote(DB.at[src, o // nx, o % nx], DB.at[dst, o // nx, o % nx], msend.at[dst, o], mrecv.at[dst, o], (p, tpp(i))))
        return res

    def blend(i):
        row = KR[pl.ds(i, 1)][0, 0:1]
        for n in range(1, n_ep):
            o = lax.rem(p + n, n_ep)
            block = jnp.dot(onehot(row), DB[pl.ds(i, 1), o // nx, o % nx][0], preferred_element_type=F32)
            X[o // nx, o % nx, rows_of(i), pl.ds(wa, wb)] = block.astype(BF16)

    def start(copies):
        for c in copies:
            c.start()

    def sent(copies):
        for c in copies:
            c.wait_send()

    def recv(copies):
        for c in copies:
            c.wait_recv()

    def send_keys(i, _):
        keys(i).start()
        return 0

    lax.fori_loop(1, n_tp, send_keys, 0)
    for j in range(cols):

        @pl.when(z < nz - 1)
        def _():
            right(q, j).start()

        @pl.when(z > 0)
        def _():
            left(q, j).start()

        share(q, j).start()
        for g in range(1, grp):
            select(g, j)
        if j == 0 and grp == 1:
            move(start, 0, 0, True)
            if wb:
                start(d1(0, True))
    if grp > 1:
        move(start, 0, 0, True)
    for j in range(1, n_ep):
        gcopy(j).start()
    acc[...] = jnp.zeros_like(acc)

    def crows(c):
        return pl.ds(pl.multiple_of(c * crow, crow), crow)

    def hidden(c):
        total = jnp.zeros((crow, 1), F32)
        for a in range(ny):
            for b in range(nx):
                v = X[a, b, crows(c)].astype(F32)
                total = total + jnp.sum(v * v, axis=1, keepdims=True)
        scale = lax.rsqrt(total / width + epsilon)
        for a in range(ny):
            for b in range(nx):
                o = a * nx + b
                v = X[a, b, crows(c)].astype(F32) * scale * G[o, 0:1]
                V[:, o * wl : (o + 1) * wl] = v.astype(BF16)
        gate = jnp.dot(V[...], WT[0], preferred_element_type=F32)
        up = jnp.dot(V[...], WT[1], preferred_element_type=F32)
        H[y, x, crows(c)] = (gate / (1.0 + jnp.exp(-gate)) * up).astype(BF16)

    def down(c):
        res = jnp.zeros((crow, wl), F32)
        for a in range(ny):
            for b in range(nx):
                o = a * nx + b
                res = res + jnp.dot(H[a, b, crows(c)], wdv[o * fl : (o + 1) * fl, :], preferred_element_type=F32)
        return res.astype(BF16)

    def combine(i):
        e = tpp(i)
        lane = lax.broadcasted_iota(jnp.int32, (T, 128), 1)
        weight = jnp.sum(jnp.where(lane == e, wcol[...], 0.0), axis=1, keepdims=True)
        term = lax.dot_general(pick(e), R[i], (((0,), (0,)), ((), ())), preferred_element_type=F32)
        acc[...] += weight * term

    def step(t, _):
        if wb:

            @pl.when(t == 3)
            def _():
                recv(d1(0, False))
                start(d2(0, True))

            @pl.when(t == 5)
            def _():
                recv(d2(0, False))
                start(pass_on(0, 1, 1))

            @pl.when(t == 9)
            def _():
                start(pass_on(0, 2, 2))

        @pl.when((t >= 6) & (t < nch + 6))
        def _():
            @pl.when(t == 6)
            def _():
                for j in range(1, n_ep):
                    gwait(j).wait_recv()

            c = hchunk(t - 6)
            move(recv, 1, c, False)
            if wb:

                @pl.when((c // cut < early) & (c % cut == 0))
                def _():
                    u = c // cut

                    @pl.when(u == 1)
                    def _():
                        recv(pass_on(0, 1, 1))

                    @pl.when(u == 2)
                    def _():
                        recv(pass_on(0, 2, 2))
                        start(pass_on(2, 3, 1))

                    @pl.when(u == 3)
                    def _():
                        recv(pass_on(2, 3, 1))

                    blend(u)

            hidden(c)
            start(h1(c, True))

        @pl.when(t < nch)
        def _():
            @pl.when(t % cut == 0)
            def _():
                for j in range(cols):
                    fetch(t // cut, j)

            move(start, 0, xchunk(t), True)

        @pl.when((t >= 9) & (t < nch + 9))
        def _():
            @pl.when(t == 9)
            def _():
                weights[2].wait()

            c = hchunk(t - 9)
            recv(h2(c, False))
            res = down(c)
            for g in range(grp):
                i = seek(horder, (t - 9) // cut) * grp + g
                h = (t - 9) % cut
                rows = pl.ds(pl.multiple_of(h * piece, piece), piece)
                O[pl.ds(i, 1), rows] = res[g * piece : (g + 1) * piece][None]

                @pl.when(i > 0)
                def _():
                    back(i, h).start()

                @pl.when(i == 0)
                def _():
                    R[0, rows] = res[g * piece : (g + 1) * piece]

        @pl.when((t >= 17) & (t < nch + 17) & ((t - 17) % cut == cut - 1))
        def _():
            for g in range(grp):
                i = seek(horder, (t - 17) // cut) * grp + g

                @pl.when(i > 0)
                def _():
                    for h in range(cut):
                        back(i, h).wait_recv()

                combine(i)

        @pl.when((t >= 7) & (t < nch + 7))
        def _():
            c = hchunk(t - 7)
            recv(h1(c, False))
            start(h2(c, True))

        @pl.when((t >= 1) & (t < nch + 1))
        def _():
            c = xchunk(t - 1)
            move(recv, 0, c, False)
            move(start, 1, c, True)

        @pl.when(t < 5)
        def _():
            @pl.when(t == 1)
            def _():
                weights[0].wait()
                weights[1].wait()

            def turn(b, _):
                at = pl.ds(pl.multiple_of((t - 1) * (width // 4) + b * 256, 256), 256)
                WT[0, at] = wgv[:, at].T
                WT[1, at] = wuv[:, at].T
                return 0

            lax.fori_loop(0, width // 1024, turn, 0)

        return 0

    lax.fori_loop(1, nch + 17, step, 0)

    moe = acc[...]
    mine = jnp.sum(moe * moe, axis=1, keepdims=True)
    SS[pl.ds(p, 1)] = jnp.broadcast_to(mine, (T, 128)).T[0:8][None]

    def scopy(j, o):
        return remote(SS.at[o], SS.at[o], ssend.at[j - 1], srecv.at[j - 1], (lax.rem(p + j, n_ep), q))

    for j in range(1, n_ep):
        scopy(j, p).start()

    def drain_tp(i, _):
        keys(i).wait_send()
        for h in range(cut):
            back(i, h).wait_send()
        return 0

    lax.fori_loop(1, n_tp, drain_tp, 0)

    def drain_z(zs, _):
        s = zs * 2 + core
        for j in range(cols):
            share(s, j).wait_send()

            @pl.when((zs <= z) & (z < nz - 1))
            def _():
                right(s, j).wait_send()

            @pl.when((zs >= z) & (z > 0))
            def _():
                left(s, j).wait_send()

        return 0

    lax.fori_loop(0, nz, drain_z, 0)

    def drain_ep(c, _):
        move(sent, 0, c, True)
        move(sent, 1, c, True)
        sent(h1(c, True) + h2(c, True))
        return 0

    lax.fori_loop(0, nch, drain_ep, 0)
    if wb:
        sent(d1(0, True) + d2(0, True) + pass_on(0, 1, 1) + pass_on(0, 2, 2) + pass_on(2, 3, 1))
    for j in range(1, n_ep):
        gcopy(j).wait_send()
    for j in range(1, n_ep):
        scopy(j, p).wait_send()
        scopy(j, lax.rem(p - j + n_ep, n_ep)).wait_recv()
    total = SS[0]
    for o in range(1, n_ep):
        total = total + SS[o]
    column = jnp.broadcast_to(total[0:1], (128, T)).T[:, 0:1]
    out[...] = (moe * lax.rsqrt(column / width + epsilon) * og[...].astype(F32).reshape(1, wl)).astype(BF16)


def body(tokens, norm_gain, expert_ids, combine_weight, w_gate, w_up, w_down, out_gain):
    T, wl = tokens.shape
    n_ep = lax.axis_size("ep")
    n_tp = lax.axis_size("tp")
    top = expert_ids.shape[1]
    cap = 2 * top * T // n_tp
    fl = w_gate.shape[1]
    width = wl * n_ep
    root = math.isqrt(n_ep)
    ny, nx = (root, root) if root * root == n_ep else (1, n_ep)
    rows = n_tp * cap
    crow = 64
    cut = max(1, cap // crow)
    nch = rows // crow
    peers = max(1, nx - 1, ny - 1)
    cols = 2 if wl % 256 == 0 else 1
    wb = wl * 6 // 8 // 128 * 128 if cap >= crow else 0
    cfg = (n_ep, n_tp, ny, nx, cap, crow, cols, wb)
    vm = pl.BlockSpec(memory_space=pltpu.VMEM)
    anym = pl.BlockSpec(memory_space=pl.ANY)
    dma = pltpu.SemaphoreType.DMA
    return pl.pallas_call(
        functools.partial(kernel, cfg),
        out_shape=jax.ShapeDtypeStruct((T, wl), BF16),
        in_specs=[vm] * 5 + [anym] * 3,
        out_specs=vm,
        scratch_shapes=[
            pltpu.VMEM((fl, width), BF16),
            pltpu.VMEM((fl, width), BF16),
            pltpu.VMEM((fl * n_ep, wl), BF16),
            pltpu.VMEM((ny, nx, rows, wl), BF16),
            pltpu.VMEM((ny, nx, rows, fl), BF16),
            pltpu.VMEM((n_tp, T, wl), BF16),
            pltpu.VMEM((n_tp, cap, wl), BF16),
            pltpu.VMEM((n_tp, cap, wl), BF16),
            pltpu.VMEM((n_ep, 8, wl), F32),
            pltpu.VMEM((n_ep, 8, T), F32),
            pltpu.VMEM((crow, width), BF16),
            pltpu.VMEM((2, width, fl), BF16),
            pltpu.VMEM((4, ny, nx, T, wb) if wb else (8, 128), BF16),
            pltpu.VMEM((n_tp, T), F32),
            pltpu.VMEM((n_tp, 8, T), F32),
            pltpu.VMEM((n_tp, 8, T), F32),
            pltpu.VMEM((T, wl), F32),
            pltpu.VMEM((T, 128), F32),
            dma((3,)),
            dma((n_tp, cols)), dma((n_tp, cols)), dma((n_tp, cols)), dma((n_tp, cols)),
            dma((n_tp, cols)), dma((n_tp, cols)), dma((n_tp,)), dma((n_tp,)),
            dma((n_tp, cut)), dma((n_tp, cut)),
            dma((n_ep,)), dma((n_ep,)), dma((n_ep,)), dma((n_ep,)),
            dma((4, nch, peers, 1)), dma((4, nch, peers, 1)), dma((4, nch, peers, 1)), dma((4, nch, peers, 1)),
            dma((4, 1, peers, 1)), dma((4, 1, peers, 1)), dma((4, n_ep)), dma((4, n_ep)),
        ],
        compiler_params=pltpu.CompilerParams(
            collective_id=0, has_side_effects=True, vmem_limit_bytes=60 * 1024 * 1024
        ),
        name="moe",
    )(
        tokens, norm_gain, expert_ids.T, combine_weight.T, out_gain,
        w_gate, w_up, w_down,
    )


def solution(mesh):
    return jax.shard_map(
        body,
        mesh=mesh,
        in_specs=(
            P("tp", "ep"),
            P("ep"),
            P("tp", None),
            P("tp", None),
            P("tp", "ep", None),
            P("tp", "ep", None),
            P("tp", None, "ep"),
            P("ep"),
        ),
        out_specs=P("tp", "ep"),
        check_vma=False,
    )
```
